32 devices in a mesh: kv: 8 (over z, y), tp: 4 (over x, core).
Axes of the slice: x: 2, y: 2, z: 4, core: 2. Of those that a mesh axis runs over, the one named last changes fastest.
Arguments:
- queries: bfloat16 [6144, 2048], P('kv', 'tp'), may hold values from -6 to 6
- keys_values: bfloat16 [6144, 1024], P('kv', 'tp'), may hold values from -6 to 6
- log_sums: float32 [6144, 32], P('kv', 'tp'), may hold values from 6.5 to 7.5
- out_grad: bfloat16 [6144, 2048], P('kv', 'tp'), may hold values from -96 to 96
- inputs: bfloat16 [6144, 4096], P('kv'), may hold values from -0.046875 to 0.046875
- chosen: int32 [48, 16], P('kv'), may hold values from -1 to 95, as said below
Outputs:
- query_grad: bfloat16 [6144, 2048], P('kv', 'tp')
- kv_grad: float32 [6144, 1024], P('kv', 'tp')
- weight_grad: float32 [4096, 2048], P('kv', 'tp')
The draws below stay inside these ranges and needn't reach their ends.
Inputs may be any that keep to these rules, and one draw needn't show every extreme that they name: `chosen`: each row names distinct key blocks, none starting after the last position of that row's query block, and -1 in unused entries; at least half of 16 blocks are named where that many are allowed. From the query blocks of one index of kv, at most 6 distinct blocks of the 768 positions of any one index are named, and this most is reached on every index.
All inputs are finite; a program needn't handle non-finite values.
Results may differ from the reference program's by a relative error of at most 0.0051.
Values may be sent and summed in bfloat16 or wider, within the bound.
A program may use at most 128 MiB of HBM per device.

```python
import jax
import jax.numpy as jnp
from jax import lax

D = 4096
H = 32
KVH = 8
DH = 64
BLK = 64
QB = 128
NSEL = 16
TOK_DEV = 768
TOKENS = 6144


def draw_chosen(key, part):
    device_count = TOKENS // TOK_DEV
    query_per = TOK_DEV // QB
    block_per = TOK_DEV // BLK
    block_total = TOKENS // BLK
    query_total = TOKENS // QB
    capacity = block_per // 2
    key_order, key_pop, key_jitter, key_count = jax.random.split(key, 4)
    order_keys = jax.random.randint(key_order, (device_count, device_count, block_per), 0, 1 << 16) * block_per + jnp.arange(block_per, dtype=jnp.int32)
    order_rank = jnp.argsort(jnp.argsort(order_keys, axis=-1, stable=True), axis=-1, stable=True)
    allowed = order_rank < capacity
    popular = jax.random.randint(key_pop, (device_count,), 0, 4)
    jitter = jax.random.randint(key_jitter, (query_total, block_total), 0, 1024)
    counts = jax.random.randint(key_count, (query_total,), NSEL // 2, NSEL + 1)
    block_ids = jnp.arange(block_total, dtype=jnp.int32)
    owner_dev = block_ids // block_per
    within = block_ids % block_per
    query_ids = jnp.arange(query_total, dtype=jnp.int32)
    device = query_ids // query_per
    local_blk = query_ids % query_per
    allow_rows = allowed[device[:, None], owner_dev[None, :], within[None, :]]
    first_rank = order_rank[device[:, None], owner_dev[None, :], within[None, :]] == 0
    causal = (block_ids * BLK)[None, :] <= (query_ids * QB + QB - 1)[:, None]
    eligible = allow_rows & causal & (owner_dev[None, :] <= device[:, None])
    last_block = (local_blk == query_per - 1)[:, None]
    own_dev = owner_dev[None, :] == device[:, None]
    before_dev = owner_dev[None, :] == device[:, None] - 1
    half_dev = owner_dev[None, :] == device[:, None] - device_count // 2
    forced = last_block & eligible & (own_dev | first_rank & (before_dev | half_dev))
    block_score = jitter + popular[owner_dev][None, :] * 1024 + forced.astype(jnp.int32) * 8192
    block_score = jnp.where(eligible, block_score, -1)
    composite = block_score * block_total + block_ids[None, :]
    top_values, top_blocks = lax.top_k(composite, NSEL)
    listed = (jnp.arange(NSEL, dtype=jnp.int32)[None, :] < counts[:, None]) & (top_values >= 0)
    return jnp.where(listed, top_blocks, -1).astype(jnp.int32)


def with_spikes(entries, key, source, target, blocks, factor):
    def block_of(dim):
        return (jnp.arange(entries.shape[dim]) // (entries.shape[dim] // blocks)).reshape((-1,) + (1,) * (entries.ndim - 1 - dim))

    near = jax.random.permutation(key, blocks)[block_of(target)]
    far = (block_of(target) + blocks // 2) % blocks
    return jnp.where((block_of(source) == near) | (block_of(source) == far), factor * entries, entries)


def block_scale(rng, shape, cuts, smallest, top_value):
    gain = 1.0
    for axis_at, shards_of in cuts:
        steps = jax.random.uniform(jax.random.fold_in(jax.random.fold_in(rng, 6), axis_at), (shards_of,), jnp.float32, smallest / len(cuts), top_value / len(cuts))
        gain = gain * jnp.repeat(jnp.exp(steps), shape[axis_at] // shards_of).reshape((-1,) + (1,) * (len(shape) - 1 - axis_at))
    return gain


def normal_values(own_key, extent, width, reach, cuts=(), kind=jnp.bfloat16):
    result = jax.random.normal(own_key, extent, jnp.float32) * width
    if len(cuts) > 0:
        result = block_scale(own_key, extent, cuts, -0.22, 0.18) * result
    return jnp.clip(result, min=-reach, max=reach).astype(kind)


def gaussian_with(rng, extent, spread, bound, shards, heavy, kind=jnp.bfloat16):
    values = spread * jax.random.normal(rng, extent, jnp.float32)
    if shards:
        values = values * block_scale(rng, extent, shards, -0.22, 0.18)
    return jnp.clip(with_spikes(values, jax.random.fold_in(rng, 3), *heavy), -bound, bound).astype(kind)


def setup_inputs(seed: int = 0) -> dict:
    key_list = jax.random.split(jax.random.key(seed), 7)
    return {
        "queries": normal_values(key_list[0], (TOKENS, H * DH), 1.0, 6.0, ((0, 8), (1, 4))),
        "keys_values": normal_values(key_list[1], (TOKENS, 2 * KVH * DH), 1.0, 6.0, ((0, 8), (1, 4))),
        "log_sums": jnp.clip(6.5 + 1.0 * jax.random.uniform(key_list[2], (TOKENS, H), jnp.float32) ** block_scale(key_list[2], (TOKENS, H), ((0, 8), (1, 4)), -0.2, 0.2), 6.5, 7.5),
        "out_grad": normal_values(key_list[3], (TOKENS, H * DH), 16.0, 96.0, ((0, 8), (1, 4))),
        "inputs": gaussian_with(key_list[4], (TOKENS, D), 0.0078125, 0.046875, ((0, 8),), (0, 1, 8, 2.0)),
        "chosen": draw_chosen(jax.random.fold_in(key_list[6], 71), 0),
    }


def reference(queries, keys_values, log_sums, out_grad, inputs, chosen):
    score_scale = DH ** -0.5
    group_size = H // KVH
    block_total = TOKENS // BLK
    row_width = 2 * KVH * DH
    kv_blocks = keys_values.reshape(block_total, BLK, KVH, 2, DH)

    def one_block(grad_table, block_index):
        row_start = block_index * QB
        query_blk = lax.dynamic_slice_in_dim(queries, row_start, QB, 0).astype(jnp.float32).reshape(QB, KVH, group_size, DH)
        grad_blk = lax.dynamic_slice_in_dim(out_grad, row_start, QB, 0).astype(jnp.float32).reshape(QB, KVH, group_size, DH)
        sums_blk = lax.dynamic_slice_in_dim(log_sums, row_start, QB, 0).reshape(QB, KVH, group_size)
        chosen_row = lax.dynamic_index_in_dim(chosen, block_index, 0, keepdims=False)
        present = chosen_row >= 0
        safe_row = jnp.maximum(chosen_row, 0).astype(jnp.int32)
        picked = kv_blocks[safe_row].astype(jnp.float32)
        key_blk = picked[:, :, :, 0, :].reshape(NSEL * BLK, KVH, DH)
        value_blk = picked[:, :, :, 1, :].reshape(NSEL * BLK, KVH, DH)
        key_pos = (safe_row[:, None] * BLK + jnp.arange(BLK, dtype=jnp.int32)[None, :]).reshape(-1)
        key_live = jnp.repeat(present, BLK)
        query_pos = row_start + jnp.arange(QB, dtype=jnp.int32)
        visible = key_live[None, :] & (key_pos[None, :] <= query_pos[:, None])
        scores = jnp.einsum('qhgd,nhd->qhgn', query_blk, key_blk) * score_scale
        attn_prob = jnp.where(visible[:, None, None, :], jnp.exp(scores - sums_blk[..., None]), jnp.float32(0.0))
        prob_round = lax.optimization_barrier(attn_prob.astype(jnp.bfloat16)).astype(jnp.float32)
        output = jnp.einsum('qhgn,nhd->qhgd', prob_round, value_blk)
        delta_row = jnp.sum(grad_blk * output, axis=-1)
        prob_grad = jnp.einsum('qhgd,nhd->qhgn', grad_blk, value_blk)
        score_grad = attn_prob * (prob_grad - delta_row[..., None])
        score_round = lax.optimization_barrier(score_grad.astype(jnp.bfloat16)).astype(jnp.float32)
        query_part = (score_scale * jnp.einsum('qhgn,nhd->qhgd', score_round, key_blk)).astype(jnp.bfloat16)
        key_part = score_scale * jnp.einsum('qhgn,qhgd->nhd', score_round, query_blk)
        value_part = jnp.einsum('qhgn,qhgd->nhd', prob_round, grad_blk)
        both_parts = jnp.stack([key_part, value_part], axis=2).reshape(NSEL, BLK, row_width)
        grad_table = grad_table.at[safe_row].add(both_parts)
        return grad_table, query_part.reshape(QB, H * DH)

    start_table = jnp.zeros((block_total, BLK, row_width), jnp.float32)
    grad_table, query_parts = lax.scan(one_block, start_table, jnp.arange(TOKENS // QB, dtype=jnp.int32))
    query_grad = query_parts.reshape(TOKENS, H * DH)
    kv_grad = grad_table.reshape(TOKENS, row_width)
    weight_grad = jnp.dot(inputs.T, query_grad, preferred_element_type=jnp.float32)
    return query_grad, kv_grad, weight_grad
```

```python
import functools

import jax
import jax.numpy as jnp
from jax import lax
from jax.experimental import pallas as pl
from jax.experimental.pallas import tpu as pltpu
from jax.sharding import PartitionSpec as P

DH = 64
BLK = 64
QB = 128
NSEL = 16
CHUNK = 4
SCALE = DH ** (-0.5)


def attend(group_size, slot_ref, chosen_ref, base_ref, tab_ref, w1_ref, w2_ref, ls_ref, dq_ref, g_ref,
           kv_scr, p_scr, dp_scr, a_scr):
    qb = pl.program_id(1)
    lanes = group_size * QB
    rows = CHUNK * BLK

    @pl.when(qb == 0)
    def _():
        g_ref[...] = jnp.zeros_like(g_ref)

    starts = [pl.multiple_of(slot_ref[qb, j] * BLK, BLK) for j in range(NSEL)]
    for j in range(NSEL):
        kv_scr[j * BLK:(j + 1) * BLK, :] = tab_ref[pl.ds(starts[j], BLK), :]
    lane = lax.broadcasted_iota(jnp.int32, (1, lanes), 1)
    qpos = (base_ref[0] + qb) * QB + lax.rem(lane, QB)
    within = lax.broadcasted_iota(jnp.int32, (BLK, lanes), 0)
    sums = ls_ref[0, 0]
    delta = jnp.zeros((1, lanes), jnp.float32)
    for c in range(NSEL // CHUNK):
        kv = kv_scr[c * rows:(c + 1) * rows, :]
        scores = jnp.dot(kv, w1_ref[0, 0, :, :lanes], preferred_element_type=jnp.float32)
        grads = jnp.dot(kv, w1_ref[0, 0, :, lanes:], preferred_element_type=jnp.float32)
        for i in range(CHUNK):
            block = chosen_ref[qb, c * CHUNK + i]
            last = jnp.where(block >= 0, qpos - block * BLK, -1)
            here = slice(i * BLK, (i + 1) * BLK)
            there = slice(c * rows + i * BLK, c * rows + (i + 1) * BLK)
            prob = jnp.where(within <= last, jnp.exp(scores[here] - sums), jnp.float32(0.0))
            rounded = prob.astype(jnp.bfloat16)
            delta += jnp.sum(rounded.astype(jnp.float32) * grads[here], axis=0, keepdims=True)
            p_scr[there, :] = prob
            dp_scr[there, :] = grads[here]
            a_scr[there, lanes:] = rounded
    for c in range(NSEL // CHUNK):
        there = slice(c * rows, (c + 1) * rows)
        a_scr[there, :lanes] = (p_scr[there, :] * (dp_scr[there, :] - delta)).astype(jnp.bfloat16)
        both = jnp.dot(a_scr[there, :], w2_ref[0, 0], preferred_element_type=jnp.float32)
        for i in range(CHUNK):
            at = pl.ds(starts[c * CHUNK + i], BLK)
            g_ref[at, :] = g_ref[at, :] + both[i * BLK:(i + 1) * BLK]
    dq_t = jnp.dot(kv_scr[...].T, a_scr[:, :lanes], preferred_element_type=jnp.float32)[:DH] * SCALE
    stacked = jnp.concatenate([dq_t[:, g * QB:(g + 1) * QB] for g in range(group_size)], axis=0)
    dq_ref[...] = stacked.T.astype(jnp.bfloat16)


def gather_sum(target_ref, part_ref, out_ref):
    out_ref[...] = jnp.zeros_like(out_ref)

    def step(i, carry):
        target = target_ref[i]

        @pl.when(target >= 0)
        def _():
            at = pl.ds(pl.multiple_of(target * BLK, BLK), BLK)
            frm = pl.ds(pl.multiple_of(i * BLK, BLK), BLK)
            out_ref[at, :] = out_ref[at, :] + part_ref[frm, :].astype(jnp.float32)

        return carry

    lax.fori_loop(0, target_ref.shape[0], step, 0)


def shards(queries, keys_values, log_sums, out_grad, inputs, chosen):
    tok_count = queries.shape[0]
    heads_here = queries.shape[1] // DH
    kv_heads = keys_values.shape[1] // (2 * DH)
    group_size = heads_here // kv_heads
    row_width = keys_values.shape[1]
    blocks_here = tok_count // BLK
    query_blocks = tok_count // QB
    kv_count = lax.axis_size("kv")
    first_block = lax.axis_index("kv") * query_blocks
    capacity = blocks_here // 2
    total_blocks = kv_count * blocks_here
    lanes = group_size * QB
    flat_ids = chosen.reshape(-1)
    needed = jnp.any(
        flat_ids[:, None] == jnp.arange(total_blocks, dtype=jnp.int32)[None, :], axis=0
    )
    needed = needed.reshape(kv_count, blocks_here).astype(jnp.int32)
    rank_in = jnp.cumsum(needed, axis=1) - 1
    matches = (needed[:, :, None] == 1) & (
        rank_in[:, :, None] == jnp.arange(capacity, dtype=jnp.int32)[None, None, :]
    )
    request = jnp.sum(
        matches.astype(jnp.int32) * jnp.arange(blocks_here, dtype=jnp.int32)[None, :, None], axis=1
    )
    request = jnp.where(jnp.any(matches, axis=1), request, -1)
    slot_flat = (jnp.arange(kv_count, dtype=jnp.int32)[:, None] * capacity + rank_in).reshape(-1)
    one_hot = chosen[:, :, None] == jnp.arange(total_blocks, dtype=jnp.int32)[None, None, :]
    slot_ids = jnp.sum(jnp.where(one_hot, slot_flat[None, None, :], 0), axis=2)
    asked_ids = lax.all_to_all(request, "kv", split_axis=0, concat_axis=0, tiled=True)
    local_blocks = keys_values.reshape(blocks_here, BLK, row_width)
    fetched = local_blocks[jnp.maximum(asked_ids, 0)]
    key_table = lax.all_to_all(fetched, "kv", split_axis=0, concat_axis=0, tiled=True).reshape(
        kv_count * capacity * BLK, row_width
    )

    def heads_first(rows):
        split = rows.reshape(query_blocks, QB, kv_heads, group_size, DH)
        return split.transpose(0, 2, 3, 1, 4).reshape(query_blocks, kv_heads, lanes, DH)

    query_rows = heads_first(queries * jnp.bfloat16(SCALE))
    grad_rows = heads_first(out_grad)
    pad = ((0, 0), (0, 0), (0, 0))
    w2 = jnp.concatenate(
        [jnp.pad(query_rows, pad + ((0, DH),)), jnp.pad(grad_rows, pad + ((DH, 0),))], axis=2
    )
    w1 = w2.swapaxes(2, 3)
    sums = (
        log_sums.reshape(query_blocks, QB, kv_heads, group_size)
        .transpose(0, 2, 3, 1)
        .reshape(query_blocks, kv_heads, 1, lanes)
    )
    table_rows = kv_count * capacity * BLK
    keys = NSEL * BLK
    query_grad, grad_table = pl.pallas_call(
        functools.partial(attend, group_size),
        grid_spec=pltpu.PrefetchScalarGridSpec(
            num_scalar_prefetch=3,
            grid=(kv_heads, query_blocks),
            in_specs=[
                pl.BlockSpec((table_rows, 2 * DH), lambda h, q, *_: (0, h)),
                pl.BlockSpec((1, 1, 2 * DH, 2 * lanes), lambda h, q, *_: (q, h, 0, 0)),
                pl.BlockSpec((1, 1, 2 * lanes, 2 * DH), lambda h, q, *_: (q, h, 0, 0)),
                pl.BlockSpec((1, 1, 1, lanes), lambda h, q, *_: (q, h, 0, 0)),
            ],
            out_specs=[
                pl.BlockSpec((QB, group_size * DH), lambda h, q, *_: (q, h)),
                pl.BlockSpec((table_rows, 2 * DH), lambda h, q, *_: (0, h)),
            ],
            scratch_shapes=[
                pltpu.VMEM((keys, 2 * DH), jnp.bfloat16),
                pltpu.VMEM((keys, lanes), jnp.float32),
                pltpu.VMEM((keys, lanes), jnp.float32),
                pltpu.VMEM((keys, 2 * lanes), jnp.bfloat16),
            ],
        ),
        out_shape=[
            jax.ShapeDtypeStruct((tok_count, heads_here * DH), jnp.bfloat16),
            jax.ShapeDtypeStruct((table_rows, row_width), jnp.float32),
        ],
        compiler_params=pltpu.CompilerParams(
            dimension_semantics=("arbitrary", "arbitrary"), vmem_limit_bytes=48 * 1024 * 1024
        ),
        cost_estimate=pl.CostEstimate(
            flops=12 * query_blocks * QB * keys * heads_here * DH,
            bytes_accessed=16 * 1024 * 1024,
            transcendentals=query_blocks * QB * keys * heads_here,
        ),
    )(slot_ids, chosen, first_block[None].astype(jnp.int32), key_table, w1, w2, sums)
    weight_part = lax.dot_general(
        inputs, query_grad, (((0,), (0,)), ((), ())), preferred_element_type=jnp.float32
    ).astype(jnp.bfloat16)
    weight_grad = lax.psum_scatter(weight_part, "kv", scatter_dimension=0, tiled=True).astype(
        jnp.float32
    )
    returned = lax.all_to_all(
        grad_table.astype(jnp.bfloat16).reshape(kv_count, capacity * BLK, row_width),
        "kv",
        split_axis=0,
        concat_axis=0,
        tiled=True,
    ).reshape(table_rows, row_width)
    kv_grad = pl.pallas_call(
        gather_sum,
        in_specs=[
            pl.BlockSpec(memory_space=pltpu.SMEM),
            pl.BlockSpec(memory_space=pltpu.VMEM),
        ],
        out_specs=pl.BlockSpec(memory_space=pltpu.VMEM),
        out_shape=jax.ShapeDtypeStruct((tok_count, row_width), jnp.float32),
    )(asked_ids.reshape(-1), returned)
    return (query_grad, kv_grad, weight_grad)


def solution(mesh):
    in_specs = (
        P("kv", "tp"),
        P("kv", "tp"),
        P("kv", "tp"),
        P("kv", "tp"),
        P("kv", None),
        P("kv", None),
    )
    out_specs = (P("kv", "tp"), P("kv", "tp"), P("kv", "tp"))
    return jax.shard_map(shards, mesh=mesh, in_specs=in_specs, out_specs=out_specs, check_vma=False)
```

```python
import functools

import jax
import jax.numpy as jnp
from jax import lax
from jax.experimental import pallas as pl
from jax.experimental.pallas import tpu as pltpu
from jax.sharding import PartitionSpec as P


DH = 64
BLK = 64
QB = 128
NSEL = 16
CHUNK = 4
SCALE = DH ** (-0.5)


def attend(group_size, parts, slot_ref, chosen_ref, base_ref, *refs):
    tab_refs, refs = refs[:parts], refs[parts:]
    w1_ref, w2_ref, ls_ref, dq_ref = refs[:4]
    g_refs, (tab_scr, g_scr, kv_scr, p_scr, dp_scr, a_scr) = refs[4:4 + parts], refs[4 + parts:]
    qb = pl.program_id(0)
    lanes = group_size * QB
    rows = CHUNK * BLK
    span = tab_refs[0].shape[0]

    @pl.when(qb == 0)
    def _():
        g_scr[...] = jnp.zeros_like(g_scr)
        for i in range(parts):
            tab_scr[i * span:(i + 1) * span, :] = tab_refs[i][...]

    starts = [pl.multiple_of(slot_ref[qb, j] * BLK, BLK) for j in range(NSEL)]
    for j in range(NSEL):
        kv_scr[j * BLK:(j + 1) * BLK, :] = tab_scr[pl.ds(starts[j], BLK), :]
    lane = lax.broadcasted_iota(jnp.int32, (1, lanes), 1)
    qpos = (base_ref[0] + qb) * QB + lax.rem(lane, QB)
    within = lax.broadcasted_iota(jnp.int32, (BLK, lanes), 0)
    sums = ls_ref[0]
    delta = jnp.zeros((1, lanes), jnp.float32)
    for c in range(NSEL // CHUNK):
        kv = kv_scr[c * rows:(c + 1) * rows, :]
        scores = jnp.dot(kv, w1_ref[0, :, :lanes], preferred_element_type=jnp.float32)
        grads = jnp.dot(kv, w1_ref[0, :, lanes:], preferred_element_type=jnp.float32)
        for i in range(CHUNK):
            block = chosen_ref[qb, c * CHUNK + i]
            last = jnp.where(block >= 0, qpos - block * BLK, -1)
            here = slice(i * BLK, (i + 1) * BLK)
            there = slice(c * rows + i * BLK, c * rows + (i + 1) * BLK)
            prob = jnp.where(within <= last, jnp.exp(scores[here] - sums), jnp.float32(0.0))
            rounded = prob.astype(jnp.bfloat16)
            delta += jnp.sum(rounded.astype(jnp.float32) * grads[here], axis=0, keepdims=True)
            p_scr[there, :] = prob
            dp_scr[there, :] = grads[here]
            a_scr[there, lanes:] = rounded
    for c in range(NSEL // CHUNK):
        there = slice(c * rows, (c + 1) * rows)
        a_scr[there, :lanes] = (p_scr[there, :] * (dp_scr[there, :] - delta)).astype(jnp.bfloat16)
        both = jnp.dot(a_scr[there, :], w2_ref[0], preferred_element_type=jnp.float32)
        for i in range(CHUNK):
            at = pl.ds(starts[c * CHUNK + i], BLK)
            g_scr[at, :] = g_scr[at, :] + both[i * BLK:(i + 1) * BLK]
    dq_t = jnp.dot(kv_scr[...].T, a_scr[:, :lanes], preferred_element_type=jnp.float32)[:DH] * SCALE
    stacked = jnp.concatenate([dq_t[:, g * QB:(g + 1) * QB] for g in range(group_size)], axis=0)
    dq_ref[...] = stacked.T.astype(jnp.bfloat16)

    @pl.when(qb == pl.num_programs(0) - 1)
    def _():
        for i in range(parts):
            g_refs[i][...] = g_scr[i * span:(i + 1) * span, :].astype(g_refs[i].dtype)


def gather_sum(target_ref, part_ref, out_ref):
    out_ref[...] = jnp.zeros_like(out_ref)

    def step(i, carry):
        target = target_ref[i]

        @pl.when(target >= 0)
        def _():
            at = pl.ds(pl.multiple_of(target * BLK, BLK), BLK)
            frm = pl.ds(pl.multiple_of(i * BLK, BLK), BLK)
            out_ref[at, :] = out_ref[at, :] + part_ref[frm, :].astype(jnp.float32)

        return carry

    lax.fori_loop(0, target_ref.shape[0], step, 0)


def shards(queries, keys_values, log_sums, out_grad, inputs, chosen):
    tok_count = queries.shape[0]
    heads_here = queries.shape[1] // DH
    kv_heads = keys_values.shape[1] // (2 * DH)
    group_size = heads_here // kv_heads
    row_width = keys_values.shape[1]
    blocks_here = tok_count // BLK
    query_blocks = tok_count // QB
    kv_count = lax.axis_size("kv")
    first_block = lax.axis_index("kv") * query_blocks
    capacity = blocks_here // 2
    total_blocks = kv_count * blocks_here
    lanes = group_size * QB
    flat_ids = chosen.reshape(-1)
    needed = jnp.any(
        flat_ids[:, None] == jnp.arange(total_blocks, dtype=jnp.int32)[None, :], axis=0
    )
    needed = needed.reshape(kv_count, blocks_here).astype(jnp.int32)
    rank_in = jnp.cumsum(needed, axis=1) - 1
    matches = (needed[:, :, None] == 1) & (
        rank_in[:, :, None] == jnp.arange(capacity, dtype=jnp.int32)[None, None, :]
    )
    request = jnp.sum(
        matches.astype(jnp.int32) * jnp.arange(blocks_here, dtype=jnp.int32)[None, :, None], axis=1
    )
    request = jnp.where(jnp.any(matches, axis=1), request, -1)
    slot_flat = (jnp.arange(kv_count, dtype=jnp.int32)[:, None] * capacity + rank_in).reshape(-1)
    one_hot = chosen[:, :, None] == jnp.arange(total_blocks, dtype=jnp.int32)[None, None, :]
    slot_ids = jnp.sum(jnp.where(one_hot, slot_flat[None, None, :], 0), axis=2)
    asked_ids = lax.all_to_all(request, "kv", split_axis=0, concat_axis=0, tiled=True)
    local_blocks = keys_values.reshape(blocks_here, BLK, row_width)
    fetched = local_blocks[jnp.maximum(asked_ids, 0)]
    key_table = lax.all_to_all(fetched, "kv", split_axis=0, concat_axis=0, tiled=True).reshape(
        kv_count * capacity * BLK, row_width
    )

    def heads_first(rows):
        split = rows.reshape(query_blocks, QB, kv_heads, group_size, DH)
        return split.transpose(0, 2, 3, 1, 4).reshape(query_blocks, kv_heads, lanes, DH)

    query_rows = heads_first(queries * jnp.bfloat16(SCALE))
    grad_rows = heads_first(out_grad)
    pad = ((0, 0), (0, 0), (0, 0))
    w2 = jnp.concatenate(
        [jnp.pad(query_rows, pad + ((0, DH),)), jnp.pad(grad_rows, pad + ((DH, 0),))], axis=2
    )
    w1 = w2.swapaxes(2, 3)
    sums = (
        log_sums.reshape(query_blocks, QB, kv_heads, group_size)
        .transpose(0, 2, 3, 1)
        .reshape(query_blocks, kv_heads, 1, lanes)
    )
    keys = NSEL * BLK
    span = table_rows = kv_count * capacity * BLK
    base = first_block[None].astype(jnp.int32)
    query_grads, weight_grads, returned = [], [], []
    for h in range(kv_heads):
        attention = pl.pallas_call(
            functools.partial(attend, group_size, 1),
            grid_spec=pltpu.PrefetchScalarGridSpec(
                num_scalar_prefetch=3,
                grid=(query_blocks,),
                in_specs=[pl.BlockSpec((span, 2 * DH), lambda q, *_, h=h: (0, h))]
                + [
                    pl.BlockSpec((1, None, 2 * DH, 2 * lanes), lambda q, *_, h=h: (q, h, 0, 0)),
                    pl.BlockSpec((1, None, 2 * lanes, 2 * DH), lambda q, *_, h=h: (q, h, 0, 0)),
                    pl.BlockSpec((1, None, 1, lanes), lambda q, *_, h=h: (q, h, 0, 0)),
                ],
                out_specs=[pl.BlockSpec((QB, group_size * DH), lambda q, *_: (q, 0))]
                + [pl.BlockSpec((span, 2 * DH), lambda q, *_: (0, 0))],
                scratch_shapes=[
                    pltpu.VMEM((span, 2 * DH), jnp.bfloat16),
                    pltpu.VMEM((span, 2 * DH), jnp.float32),
                    pltpu.VMEM((keys, 2 * DH), jnp.bfloat16),
                    pltpu.VMEM((keys, lanes), jnp.float32),
                    pltpu.VMEM((keys, lanes), jnp.float32),
                    pltpu.VMEM((keys, 2 * lanes), jnp.bfloat16),
                ],
            ),
            out_shape=[jax.ShapeDtypeStruct((tok_count, group_size * DH), jnp.bfloat16)]
            + [jax.ShapeDtypeStruct((span, 2 * DH), jnp.bfloat16)],
            compiler_params=pltpu.CompilerParams(
                dimension_semantics=("arbitrary",), vmem_limit_bytes=40 * 1024 * 1024
            ),
            cost_estimate=pl.CostEstimate(
                flops=12 * query_blocks * QB * keys * group_size * DH,
                bytes_accessed=8 * 1024 * 1024,
                transcendentals=query_blocks * QB * keys * group_size,
            ),
        )
        outs = attention(slot_ids, chosen, base, key_table, w1, w2, sums)
        query_grads.append(outs[0])
        returned.append(outs[1])
        weight_part = lax.dot_general(
            inputs, outs[0], (((0,), (0,)), ((), ())), preferred_element_type=jnp.float32
        ).astype(jnp.bfloat16)
        weight_part, base = lax.optimization_barrier((weight_part, base))
        weight_grads.append(
            lax.psum_scatter(weight_part, "kv", scatter_dimension=0, tiled=True)
        )
    query_grad = jnp.concatenate(query_grads, axis=1)
    weight_grad = jnp.concatenate(weight_grads, axis=1).astype(jnp.float32)
    grad_table = jnp.concatenate(returned, axis=1)
    received = lax.all_to_all(
        grad_table.reshape(kv_count, capacity * BLK, row_width),
        "kv",
        split_axis=0,
        concat_axis=0,
        tiled=True,
    ).reshape(table_rows, row_width)
    kv_grad = pl.pallas_call(
        gather_sum,
        in_specs=[
            pl.BlockSpec(memory_space=pltpu.SMEM),
            pl.BlockSpec(memory_space=pltpu.VMEM),
        ],
        out_specs=pl.BlockSpec(memory_space=pltpu.VMEM),
        out_shape=jax.ShapeDtypeStruct((tok_count, row_width), jnp.float32),
    )(asked_ids.reshape(-1), received)
    return (query_grad, kv_grad, weight_grad)


def solution(mesh):
    in_specs = (
        P("kv", "tp"),
        P("kv", "tp"),
        P("kv", "tp"),
        P("kv", "tp"),
        P("kv", None),
        P("kv", None),
    )
    out_specs = (P("kv", "tp"), P("kv", "tp"), P("kv", "tp"))
    return jax.shard_map(shards, mesh=mesh, in_specs=in_specs, out_specs=out_specs, check_vma=False)
```
